32 devices in a mesh: ep: 8 (over z, y), tp: 4 (over x, core).
Axes of the slice: x: 2, y: 2, z: 4, core: 2. Of those that a mesh axis runs over, the one named last changes fastest.
Arguments:
- residual_in: bfloat16 [16, 2048], P('ep'), may hold values from -6 to 6
- gla_state: float32 [16, 4, 256, 512], P('ep', 'tp'), may hold values from -6 to 6
- norm_gain: bfloat16 [2048], replicated, may hold values from 0.099609375 to 1.8984375
- w_query: bfloat16 [2048, 1024], P('ep', 'tp'), may hold values from -0.125 to 0.125
- w_key: bfloat16 [2048, 1024], P('ep', 'tp'), may hold values from -0.125 to 0.125
- w_value: bfloat16 [2048, 2048], P('ep', 'tp'), may hold values from -0.125 to 0.125
- w_decay: bfloat16 [2048, 1024], P('ep', 'tp'), may hold values from -0.5 to 0.5
- decay_bias: float32 [1024], P('tp'), may hold values from -40 to 8
- head_gain: bfloat16 [512], replicated, may hold values from 0.099609375 to 1.8984375
- w_output: bfloat16 [2048, 2048], P('tp', 'ep'), may hold values from -0.125 to 0.125
- ffn_gain: bfloat16 [2048], replicated, may hold values from 0.099609375 to 1.8984375
- router_group: bfloat16 [2048, 4], replicated, may hold values from -0.125 to 0.125
- router_expert: bfloat16 [8, 2048], replicated, may hold values from -0.125 to 0.125
- expert_ids: int32 [16, 2], replicated, may hold values from 0 to 7, all different within a row; in each aligned block of 16 rows (0 to 15, 16 to 31, ...) at most 16 rows name the same one
- w_gate: bfloat16 [8, 2048, 512], P('ep', None, 'tp'), may hold values from -0.125 to 0.125
- w_up: bfloat16 [8, 2048, 512], P('ep', None, 'tp'), may hold values from -0.125 to 0.125
- w_down: bfloat16 [8, 512, 2048], P('ep', 'tp'), may hold values from -0.75 to 0.75
Outputs:
- layer_out: bfloat16 [16, 2048], P('ep')
- new_state: float32 [16, 4, 256, 512], P('ep', 'tp')
The draws below stay inside these ranges and needn't reach their ends.
Inputs may be any that keep to these rules, and one draw needn't show every extreme that they name: `expert_ids`: each row names 2 different experts; no expert is named by more than 16 rows of the whole batch, a bound that some block reaches.
All inputs are finite; a program needn't handle non-finite values.
Results may differ from the reference program's by a relative error of at most 0.023.
Values may be sent and summed in bfloat16 or wider, within the bound.
A program may use at most 64 MiB of HBM per device.

```python
import math
import jax
import jax.numpy as jnp
import numpy as np
from jax import lax

D = 2048
HEADS = 4
DKH = 256
DVH = 512
FF = 512
GROUPS = 4
TOP = 2
TOKENS = 16
EXPERTS = 8
CAP = 16
DK = 1024
DV = 2048


def draw_decay_bias(key, part):
    return jax.random.uniform(key, (HEADS * DKH,), jnp.float32, -40.0, 8.0)


def levels(own_key, shape, cuts, least, high):
    loudness = 1.0
    for axis_at, shards_of in cuts:
        heights = jax.random.uniform(jax.random.fold_in(jax.random.fold_in(own_key, 6), axis_at), (shards_of,), jnp.float32, least / len(cuts), high / len(cuts))
        loudness = loudness * jnp.repeat(jnp.exp(heights), shape[axis_at] // shards_of).reshape((-1,) + (1,) * (len(shape) - 1 - axis_at))
    return loudness


def deal_out(own_key, own, number, rows, count, top, reach, slope):
    sequence = jax.random.permutation(own_key, count)
    crowded, usual = portions_of(count, rows * top, reach, slope, True), portions_of(count, rows * top, reach, slope, False)
    places = jnp.arange(count)

    def named(lengths, rotation):
        used = int((lengths > 0).sum())
        fixed = max(1, used // 4)
        shifted = fixed + (places - fixed + rotation * (used - fixed)) % max(1, count - fixed)
        return jnp.zeros((count,), jnp.int32).at[sequence[jnp.where(places < fixed, places, shifted)]].set(jnp.asarray(lengths, jnp.int32))

    lengths = jnp.where(number % 4 == 0, named(crowded, number // 4), named(usual, number - number // 4 - 1))
    mixed = jax.random.permutation(jax.random.fold_in(own, 3), count)
    source_of, receiver = mixed[0:count // 2 * 2:2], mixed[1:count // 2 * 2:2]
    margin = jnp.minimum(lengths[source_of] - 1, reach - lengths[receiver]) // 2
    margin = jnp.where((source_of == sequence[0]) | (receiver == sequence[0]) | (lengths[receiver] == 0), 0, jnp.maximum(margin, 0))
    shifted = jax.random.randint(jax.random.fold_in(own, 4), (count // 2,), 0, 1 << 20) % (margin + 1)
    lengths = lengths.at[source_of].add(-shifted).at[receiver].add(shifted)
    labels = jnp.searchsorted(jnp.cumsum(lengths), jnp.arange(rows * top), side="right").astype(jnp.int32)
    listing = labels.reshape(top, rows).T
    listing = listing[jax.random.permutation(jax.random.fold_in(own, 1), rows)]
    rotation = jax.random.randint(jax.random.fold_in(own, 2), (rows, 1), 0, top)
    return jnp.take_along_axis(listing, (jnp.arange(top)[None, :] + rotation) % top, axis=1)


def portions_of(amount, total, limit, lean, full):
    portions = [(1 << 20) // math.isqrt(rank ** lean) + 1 for rank in range(1, amount + 1)]
    largest = limit if full else min(limit, max(-(-total // amount), total * portions[0] // sum(portions)))
    least = 1 if total - largest >= amount - 1 else 0
    holding, surplus = [largest] + [least] * (amount - 1), total - largest - least * (amount - 1)
    while surplus > 0:
        candidates = [i for i in range(1, amount) if holding[i] < largest] or [i for i in range(1, amount) if holding[i] < limit]
        pool, remaining = sum([portions[i] for i in candidates]), surplus
        for i in candidates:
            addition = min(limit - holding[i], max(1, remaining * portions[i] // pool), surplus)
            holding[i] = holding[i] + addition
            surplus = surplus - addition
    return np.array(holding)


def normal_values(rng, extent, scale, bound, shards=(), kind=jnp.bfloat16):
    array = scale * jax.random.normal(rng, extent, jnp.float32)
    if shards:
        array = array * levels(rng, extent, shards, -0.22, 0.18)
    return jnp.clip(array, -bound, bound).astype(kind)


def setup_inputs(seed: int = 0) -> dict:
    arg_keys = jax.random.split(jax.random.key(seed), 18)
    residual_in = normal_values(arg_keys[0], (TOKENS, D), 1.0, 6.0, ((0, 8),))
    gla_state = normal_values(arg_keys[1], (TOKENS, HEADS, DKH, DVH), 1.0, 6.0, ((0, 8), (1, 4)), jnp.float32)
    norm_gain = jnp.clip(1.0 + 0.18 * jax.random.normal(arg_keys[2], (D,), jnp.float32), 0.099609375, 1.8984375).astype(jnp.bfloat16)
    w_query = normal_values(arg_keys[3], (D, DK), D ** -0.5, 0.125, ((0, 8), (1, 4)))
    w_key = normal_values(arg_keys[4], (D, DK), D ** -0.5, 0.125, ((0, 8), (1, 4)))
    w_value = normal_values(arg_keys[5], (D, DV), D ** -0.5, 0.125, ((0, 8), (1, 4)))
    w_decay = normal_values(arg_keys[6], (D, DK), (4 * D ** -0.5), 0.5, ((0, 8), (1, 4)))
    decay_bias = draw_decay_bias(jax.random.fold_in(arg_keys[17], 71), 0)
    head_gain = jnp.clip(1.0 + 0.18 * jax.random.normal(arg_keys[8], (DVH,), jnp.float32), 0.099609375, 1.8984375).astype(jnp.bfloat16)
    w_output = normal_values(arg_keys[9], (DV, D), DV ** -0.5, 0.125, ((0, 4), (1, 8)))
    ffn_gain = jnp.clip(1.0 + 0.18 * jax.random.normal(arg_keys[10], (D,), jnp.float32), 0.099609375, 1.8984375).astype(jnp.bfloat16)
    router_group = normal_values(arg_keys[11], (D, GROUPS), D ** -0.5, 0.125)
    router_expert = normal_values(arg_keys[12], (EXPERTS, D), D ** -0.5, 0.125)
    expert_ids_keys = jax.random.split(jax.random.fold_in(arg_keys[13], 1), TOKENS // TOKENS)
    expert_ids_turns = jax.random.permutation(jax.random.fold_in(arg_keys[13], 3), TOKENS // TOKENS)
    expert_ids = jax.vmap(lambda own, number: deal_out(jax.random.fold_in(arg_keys[13], 2), own, number, TOKENS, EXPERTS, TOP, CAP, 2))(expert_ids_keys, expert_ids_turns).reshape((TOKENS, TOP))
    w_gate = normal_values(arg_keys[14], (EXPERTS, D, FF), D ** -0.5, 0.125, ((0, 8), (2, 4)))
    w_up = normal_values(arg_keys[15], (EXPERTS, D, FF), D ** -0.5, 0.125, ((0, 8), (2, 4)))
    w_down = normal_values(arg_keys[16], (EXPERTS, FF, D), (3 * FF ** -0.5), 0.75, ((0, 8), (1, 4)))
    return {"residual_in": residual_in, "gla_state": gla_state, "norm_gain": norm_gain, "w_query": w_query, "w_key": w_key, "w_value": w_value, "w_decay": w_decay, "decay_bias": decay_bias, "head_gain": head_gain, "w_output": w_output, "ffn_gain": ffn_gain, "router_group": router_group, "router_expert": router_expert, "expert_ids": expert_ids, "w_gate": w_gate, "w_up": w_up, "w_down": w_down}


EPSILON = 1e-06
GATE_SCALE = 16.0

def rms_scale(values, gain_vec):
    floats = values.astype(jnp.float32)
    return floats * lax.rsqrt(lax.optimization_barrier(jnp.mean(floats * floats, axis=-1, keepdims=True)) + EPSILON) * gain_vec.astype(jnp.float32)

def reference(residual_in, gla_state, norm_gain, w_query, w_key, w_value, w_decay, decay_bias, head_gain, w_output, ffn_gain, router_group, router_expert, expert_ids, w_gate, w_up, w_down):
    tokens = residual_in.shape[0]
    normed = rms_scale(residual_in, norm_gain).astype(jnp.bfloat16)
    query_rows = jnp.dot(normed, w_query, preferred_element_type=jnp.float32).astype(jnp.bfloat16)
    key_rows = jnp.dot(normed, w_key, preferred_element_type=jnp.float32).astype(jnp.bfloat16)
    value_rows = jnp.dot(normed, w_value, preferred_element_type=jnp.float32).astype(jnp.bfloat16)
    decay_pre = jnp.dot(normed, w_decay, preferred_element_type=jnp.float32)
    log_decay = jax.nn.log_sigmoid(decay_pre + decay_bias) / GATE_SCALE
    query_float = lax.optimization_barrier(query_rows).astype(jnp.float32).reshape(tokens, HEADS, DKH) * DKH ** (-0.5)
    key_float = lax.optimization_barrier(key_rows).astype(jnp.float32).reshape(tokens, HEADS, DKH)
    value_float = lax.optimization_barrier(value_rows).astype(jnp.float32).reshape(tokens, HEADS, DVH)
    alpha = jnp.exp(log_decay).reshape(tokens, HEADS, DKH)
    new_state = alpha[..., None] * gla_state + key_float[..., None] * value_float[:, :, None, :]
    read_out = jnp.einsum('thk,thkv->thv', query_float, new_state, precision=lax.Precision.HIGHEST)
    gated_heads = rms_scale(read_out, head_gain).astype(jnp.bfloat16)
    attention = jnp.zeros((tokens, D), jnp.float32)
    for head_index in range(HEADS):
        partial_out = jnp.dot(gated_heads[:, head_index], w_output[head_index * DVH:(head_index + 1) * DVH], preferred_element_type=jnp.float32).astype(jnp.bfloat16)
        attention = attention + lax.optimization_barrier(partial_out).astype(jnp.float32)
    hidden_res = (residual_in.astype(jnp.float32) + attention).astype(jnp.bfloat16)
    moe_in = rms_scale(hidden_res, ffn_gain).astype(jnp.bfloat16)
    group_logits = jnp.dot(moe_in, router_group, preferred_element_type=jnp.float32)
    expert_logits = jnp.dot(moe_in, router_expert.T, preferred_element_type=jnp.float32)
    per_group = EXPERTS // GROUPS

    def route_weight(mine_col, other_col):
        chosen = jnp.take_along_axis(expert_logits, expert_ids[:, mine_col:mine_col + 1], axis=1)[:, 0]
        rival_logit = jnp.take_along_axis(expert_logits, expert_ids[:, other_col:other_col + 1], axis=1)[:, 0]
        group_of = (expert_ids[:, mine_col] // per_group).astype(jnp.int32)
        group_logit = jnp.take_along_axis(group_logits, group_of[:, None], axis=1)[:, 0]
        group_share = 1.0 / lax.optimization_barrier(jnp.sum(jnp.exp(group_logits - group_logit[:, None]), axis=1))
        return group_share * jax.nn.sigmoid(chosen - rival_logit)
    weights = jnp.stack([route_weight(0, 1), route_weight(1, 0)], axis=1)
    slot_index = jnp.arange(CAP, dtype=jnp.int32)

    def expert_step(summed, expert):
        is_named = jnp.any(expert_ids == expert, axis=1)
        slot_of = jnp.cumsum(is_named.astype(jnp.int32)) - 1
        select = (is_named[None, :] & (slot_of[None, :] == slot_index[:, None])).astype(jnp.float32)
        slot_rows = jnp.dot(select.astype(jnp.bfloat16), moe_in, preferred_element_type=jnp.float32).astype(jnp.bfloat16)
        gate_out = jnp.dot(slot_rows, w_gate[expert], preferred_element_type=jnp.float32)
        up_out = jnp.dot(slot_rows, w_up[expert], preferred_element_type=jnp.float32)
        hidden = (jax.nn.silu(gate_out) * up_out).astype(jnp.bfloat16)
        output = jnp.dot(hidden, w_down[expert], preferred_element_type=jnp.float32)
        token_weight = lax.optimization_barrier(jnp.sum(jnp.where(expert_ids == expert, weights, jnp.zeros_like(weights)), axis=1))
        slot_weight = jnp.dot(select, token_weight, precision=lax.Precision.HIGHEST)
        summed = summed + jnp.dot(select.T, output * slot_weight[:, None], precision=lax.Precision.HIGHEST)
        return (summed, None)
    moe_sum, _ = lax.scan(expert_step, jnp.zeros((tokens, D), jnp.float32), jnp.arange(EXPERTS, dtype=jnp.int32))
    layer_out = (hidden_res.astype(jnp.float32) + moe_sum).astype(jnp.bfloat16)
    return (layer_out, new_state)
```

```python
import functools

import jax
import jax.numpy as jnp
from jax import lax
from jax.experimental import pallas as pl
from jax.experimental.pallas import tpu as pltpu
from jax.sharding import PartitionSpec as P

EPSILON = 1e-06
GATE_SCALE = 16.0
F32 = jnp.float32
BF16 = jnp.bfloat16
LANES = 128
MESH = pl.DeviceIdType.MESH


def mm(left, right):
    return jnp.dot(left, right, preferred_element_type=F32)


def over_peers(count, body):
    if count <= 8:
        for d in range(1, count):
            body(d)
    else:

        def step(d, carry):
            body(d)
            return carry

        lax.fori_loop(1, count, step, 0)


def over_range(count, body):
    for i in range(count):
        body(i)


def take_cols(ref, index, cols):
    if cols % LANES == 0:
        return ref[:, pl.ds(pl.multiple_of(index * cols, LANES), cols)]
    rows = ref.shape[1]
    select = (
        lax.broadcasted_iota(jnp.int32, (rows, cols), 0)
        == lax.broadcasted_iota(jnp.int32, (rows, cols), 1) + index * cols
    )
    return mm(ref[...], jnp.where(select, 1.0, 0.0).astype(BF16)).astype(BF16)


def kernel(
    n,
    t,
    residual_in,
    gla_state,
    norm_gain,
    w_query,
    w_key,
    w_value,
    w_decay,
    decay_bias,
    head_gain,
    w_output,
    ffn_gain,
    router_group,
    router_expert,
    expert_ids,
    w_gate,
    w_up,
    w_down,
    layer_out,
    new_state,
    res,
    state,
    ng,
    wcat,
    bias,
    hg,
    wo,
    fg,
    rg,
    re,
    ids,
    wgu,
    wd,
    load_sem,
    out_sem,
    a_rx,
    b_tx,
    b_rx,
    c_tx,
    c_rx,
    d1_rx,
    d1_tx,
    d2_rx,
    f1_tx,
    f1_rx,
    f2_rx,
    f2_tx,
    lout,
    rows_a,
    rows_c,
    heads8,
    proj,
    moe_out,
    ep_send,
    ep_recv,
    tp_send,
    tp_recv,
):
    e = lax.axis_index("ep")
    h = lax.axis_index("tp")
    seqs, width = res.shape
    cols = wcat.shape[0]
    kw = w_query.shape[1]
    vw = w_value.shape[1]
    tokens = n * seqs
    ff = wd.shape[0]
    aligned = cols % LANES == 0

    loads = []

    def load(src, dst):
        copy = pltpu.make_async_copy(src, dst, load_sem.at[len(loads)])
        copy.start()
        loads.append(copy)
        return copy

    ld_res = load(residual_in, res)
    ld_ng = load(norm_gain, ng)
    ld_w = [
        load(w_query, wcat.at[:, 0:kw]),
        load(w_key, wcat.at[:, kw : 2 * kw]),
        load(w_value, wcat.at[:, 2 * kw : 2 * kw + vw]),
        load(w_decay, wcat.at[:, 2 * kw + vw :]),
    ]
    ld_small = [load(decay_bias, bias), load(head_gain, hg), load(ffn_gain, fg)]
    ld_state = load(gla_state.at[:, 0], state)
    ld_wo = load(w_output, wo)
    ld_route = [load(router_group, rg), load(router_expert, re), load(expert_ids, ids)]
    ld_gu = [load(w_gate.at[0], wgu.at[:, 0:ff]), load(w_up.at[0], wgu.at[:, ff : 2 * ff])]
    ld_wd = load(w_down.at[0], wd)

    barrier = pltpu.get_barrier_semaphore()
    over_peers(
        n,
        lambda d: pl.semaphore_signal(
            barrier, inc=1, device_id={"ep": lax.rem(e + d, n)}, device_id_type=MESH
        ),
    )
    over_peers(
        t,
        lambda d: pl.semaphore_signal(
            barrier, inc=1, device_id={"tp": lax.rem(h + d, t)}, device_id_type=MESH
        ),
    )

    def ep_copy(phase, src, dst, peer, slot):
        return pltpu.make_async_remote_copy(
            src_ref=src,
            dst_ref=dst,
            send_sem=ep_send.at[phase, peer],
            recv_sem=ep_recv.at[phase, slot],
            device_id={"ep": peer},
            device_id_type=MESH,
        )

    def tp_copy(phase, src, dst, peer, slot):
        return pltpu.make_async_remote_copy(
            src_ref=src,
            dst_ref=dst,
            send_sem=tp_send.at[phase, peer],
            recv_sem=tp_recv.at[phase, slot],
            device_id={"tp": peer},
            device_id_type=MESH,
        )

    def ep_src(tx):
        return lambda peer: tx.at[peer]

    def ep_phase_send(phase, src_of, rx):
        def one(d):
            peer = lax.rem(e + d, n)
            ep_copy(phase, src_of(peer), rx.at[e], peer, e).start()

        over_peers(n, one)

    def ep_wait(phase, rx, peer):
        ep_copy(phase, rx.at[peer], rx.at[peer], peer, peer).wait_recv()

    def ep_drain(phase, src_of, rx):
        def one(d):
            peer = lax.rem(e + d, n)
            ep_copy(phase, src_of(peer), rx.at[e], peer, e).wait_send()

        over_peers(n, one)

    def tp_phase_send(phase, src, rx):
        def one(d):
            peer = lax.rem(h + d, t)
            tp_copy(phase, src, rx.at[h], peer, h).start()

        over_peers(t, one)

    def tp_wait_all(phase, rx):
        def one(d):
            peer = lax.rem(h + d, t)
            tp_copy(phase, rx.at[peer], rx.at[peer], peer, peer).wait_recv()

        over_peers(t, one)

    def tp_drain(phase, src, rx):
        def one(d):
            peer = lax.rem(h + d, t)
            tp_copy(phase, src, rx.at[h], peer, h).wait_send()

        over_peers(t, one)

    if aligned:
        a_src = lambda peer: res.at[:, pl.ds(pl.multiple_of(peer * cols, LANES), cols)]
    else:
        a_src = lambda peer: res
    ld_res.wait()
    pl.semaphore_wait(barrier, n - 1 + t - 1)
    ep_phase_send(0, a_src, a_rx)
    own = res[...]
    a_rx[e] = take_cols(res, e, cols) if aligned else own
    own_float = own.astype(F32)
    token_scale = lax.rsqrt(jnp.mean(own_float * own_float, axis=-1, keepdims=True) + EPSILON)
    ld_ng.wait()
    ng_cols = take_cols(ng, e, cols).astype(F32)
    for copy in ld_w:
        copy.wait()
    over_peers(n, lambda d: ep_wait(0, a_rx, lax.rem(e + d, n)))

    def fill_a(i):
        if aligned:
            piece = a_rx[i]
        else:
            piece = take_cols(a_rx.at[i], e, cols)
        rows_a[pl.ds(i * seqs, seqs), :] = piece.astype(F32)

    over_range(n, fill_a)

    lhs = (rows_a[...] * ng_cols).astype(BF16)
    proj[...] = mm(lhs, wcat[...])

    def fill_b(i):
        b_tx[i] = proj[pl.ds(i * seqs, seqs), :].astype(BF16)

    over_range(n, fill_b)
    ep_phase_send(1, ep_src(b_tx), b_rx)
    for copy in ld_small:
        copy.wait()
    ld_state.wait()
    b_rx[e] = b_tx[e]
    over_peers(n, lambda d: ep_wait(1, b_rx, lax.rem(e + d, n)))
    total = jnp.sum(b_rx[...].astype(F32), axis=0) * token_scale

    heads8[...] = jnp.zeros_like(heads8)
    decay_pre = total[:, 2 * kw + vw :] + bias[...]
    log_decay = (
        jnp.minimum(decay_pre, 0.0) - jnp.log1p(jnp.exp(-jnp.abs(decay_pre)))
    ) / GATE_SCALE
    heads8[0:seqs, :] = total[:, 0:kw] * kw ** (-0.5)
    heads8[seqs : 2 * seqs, :] = total[:, kw : 2 * kw]
    heads8[2 * seqs : 3 * seqs, :] = jnp.exp(log_decay)
    turned = heads8[...].T
    value_rows = total[:, 2 * kw : 2 * kw + vw]
    for b in range(seqs):
        value = value_rows[b : b + 1]
        acc = jnp.zeros((8, vw), F32)
        chunk = 64
        for c in range(0, kw, chunk):
            q_col = turned[c : c + chunk, b : b + 1]
            k_col = turned[c : c + chunk, seqs + b : seqs + b + 1]
            a_col = turned[c : c + chunk, 2 * seqs + b : 2 * seqs + b + 1]
            fresh = a_col * state[b, c : c + chunk, :] + k_col * value
            state[b, c : c + chunk, :] = fresh
            acc = acc + jnp.sum((q_col * fresh).reshape(chunk // 8, 8, vw), axis=0)
        read = jnp.sum(acc, axis=0, keepdims=True)
        gated = read * lax.rsqrt(jnp.mean(read * read, axis=-1, keepdims=True) + EPSILON)
        gated = gated * hg[...].astype(F32)
        rows_c[b : b + 1, :] = gated
    c_tx[...] = rows_c[0:seqs, :].astype(BF16)

    c_src = lambda peer: c_tx
    ep_phase_send(2, c_src, c_rx)
    st_out = pltpu.make_async_copy(state, new_state.at[:, 0], out_sem.at[0])
    st_out.start()
    c_rx[e] = c_tx[...]
    ld_wo.wait()
    over_peers(n, lambda d: ep_wait(2, c_rx, lax.rem(e + d, n)))

    def fill_c(i):
        rows_c[pl.ds(i * seqs, seqs), :] = c_rx[i].astype(F32)

    over_range(n, fill_c)

    part = mm(rows_c[...].astype(BF16), wo[...]).astype(BF16)
    d1_tx[...] = part
    tp_phase_send(0, d1_tx, d1_rx)
    d1_rx[h] = part
    tp_wait_all(0, d1_rx)
    attention = jnp.sum(d1_rx[...].astype(F32), axis=0)
    hid = (rows_a[...] + attention).astype(BF16)
    d2_rx[e] = hid
    d2_src = lambda peer: d2_rx.at[e]
    ep_phase_send(3, d2_src, d2_rx)
    for copy in ld_route + ld_gu:
        copy.wait()

    square = jnp.zeros((tokens, 1), F32)
    gate_up = jnp.zeros((tokens, 2 * ff), F32)
    group_logits = jnp.zeros((tokens, rg.shape[1]), F32)
    expert_logits = jnp.zeros((tokens, re.shape[0]), F32)

    def moe_chunk(d, carry):
        square, gate_up, group_logits, expert_logits = carry
        src = lax.rem(e + d, n)
        piece = d2_rx[src].astype(F32)
        square = square + jnp.sum(piece * piece, axis=-1, keepdims=True)
        piece = (piece * take_cols(fg, src, cols).astype(F32)).astype(BF16)
        span = pl.ds(pl.multiple_of(src * cols, cols), cols)
        gate_up = gate_up + mm(piece, wgu[span, :])
        group_logits = group_logits + mm(piece, rg[span, :])
        expert_logits = expert_logits + lax.dot_general(
            piece,
            take_cols(re, src, cols),
            (((1,), (1,)), ((), ())),
            preferred_element_type=F32,
        )
        return square, gate_up, group_logits, expert_logits

    def moe_step(d, carry):
        ep_wait(3, d2_rx, lax.rem(e + d, n))
        return moe_chunk(d, carry)

    carry = moe_chunk(0, (square, gate_up, group_logits, expert_logits))
    if n <= 8:
        for d in range(1, n):
            carry = moe_step(d, carry)
    else:
        carry = lax.fori_loop(1, n, moe_step, carry)
    square, gate_up, group_logits, expert_logits = carry
    scale = lax.rsqrt(square / (n * cols) + EPSILON)
    gate_up = gate_up * scale
    group_logits = group_logits * scale
    expert_logits = expert_logits * scale

    groups = group_logits.shape[1]
    experts = expert_logits.shape[1]
    first, second = ids[:, 0:1], ids[:, 1:2]
    named = (first == e) | (second == e)
    rival = jnp.where(first == e, second, first)
    expert_at = lax.broadcasted_iota(jnp.int32, expert_logits.shape, 1)
    group_at = lax.broadcasted_iota(jnp.int32, group_logits.shape, 1)
    pick = lambda mask, values: jnp.sum(jnp.where(mask, values, 0.0), axis=1, keepdims=True)
    chosen = pick(expert_at == e, expert_logits)
    rival_logit = pick(expert_at == rival, expert_logits)
    group_logit = pick(group_at == e // (experts // groups), group_logits)
    share = 1.0 / jnp.sum(jnp.exp(group_logits - group_logit), axis=1, keepdims=True)
    weight = jnp.where(named, share / (1.0 + jnp.exp(rival_logit - chosen)), 0.0)

    gate, up = gate_up[:, 0:ff], gate_up[:, ff : 2 * ff]
    hidden = (gate / (1.0 + jnp.exp(-gate)) * up).astype(BF16)
    ld_wd.wait()
    moe_out[...] = mm(hidden, wd[...]) * weight

    def fill_f(i):
        f1_tx[i] = moe_out[pl.ds(i * seqs, seqs), :].astype(BF16)

    over_range(n, fill_f)
    f1_src = ep_src(f1_tx)
    ep_phase_send(4, f1_src, f1_rx)
    f1_rx[e] = f1_tx[e]
    own_rows = (
        lax.broadcasted_iota(jnp.int32, (8, tokens), 1)
        == lax.broadcasted_iota(jnp.int32, (8, tokens), 0) + e * seqs
    )
    own_rows = jnp.where(own_rows, 1.0, 0.0).astype(BF16)
    if aligned:
        for i in range(n):
            lout[:, i * cols : (i + 1) * cols] = mm(own_rows, d2_rx[i])[0:seqs]
    over_peers(n, lambda d: ep_wait(4, f1_rx, lax.rem(e + d, n)))
    f2_tx[...] = jnp.sum(f1_rx[...].astype(F32), axis=0).astype(BF16)
    tp_phase_send(1, f2_tx, f2_rx)
    f2_rx[h] = f2_tx[...]
    tp_wait_all(1, f2_rx)
    if not aligned:

        def place(i, total_rows):
            rows = mm(own_rows, d2_rx[i]).astype(BF16)
            select = (
                lax.broadcasted_iota(jnp.int32, (cols, width), 1)
                == lax.broadcasted_iota(jnp.int32, (cols, width), 0) + i * cols
            )
            return total_rows + mm(rows, jnp.where(select, 1.0, 0.0).astype(BF16))

        lout[...] = lax.fori_loop(0, n, place, jnp.zeros((8, width), F32))[0:seqs]
    moe_sum = jnp.sum(f2_rx[...].astype(F32), axis=0)
    layer_out[...] = (lout[...] + moe_sum).astype(BF16)

    ep_drain(0, a_src, a_rx)
    ep_drain(1, ep_src(b_tx), b_rx)
    ep_drain(2, c_src, c_rx)
    ep_drain(3, d2_src, d2_rx)
    ep_drain(4, f1_src, f1_rx)
    tp_drain(0, d1_tx, d1_rx)
    tp_drain(1, f2_tx, f2_rx)
    st_out.wait()


def on_device(n, t, *arrays):
    (
        residual_in,
        gla_state,
        norm_gain,
        w_query,
        w_key,
        w_value,
        w_decay,
        decay_bias,
        head_gain,
        w_output,
        ffn_gain,
        router_group,
        router_expert,
        expert_ids,
        w_gate,
        w_up,
        w_down,
    ) = arrays
    seqs, width = residual_in.shape
    tokens = n * seqs
    cols, kw = w_query.shape
    vw = w_value.shape[1]
    ff = w_gate.shape[2]
    span = 3 * kw + vw
    out_cols = w_output.shape[1]
    a_cols = cols if cols % LANES == 0 else width
    row = lambda a: a.reshape(1, -1)
    operands = (
        residual_in,
        gla_state,
        row(norm_gain),
        w_query,
        w_key,
        w_value,
        w_decay,
        row(decay_bias),
        row(head_gain),
        w_output,
        row(ffn_gain),
        router_group,
        router_expert,
        expert_ids,
        w_gate,
        w_up,
        w_down,
    )
    dma = pltpu.SemaphoreType.DMA
    scratch = [
        pltpu.VMEM((seqs, width), BF16),
        pltpu.VMEM((seqs, kw, vw), F32),
        pltpu.VMEM((1, width), BF16),
        pltpu.VMEM((cols, span), BF16),
        pltpu.VMEM((1, kw), F32),
        pltpu.VMEM((1, vw), BF16),
        pltpu.VMEM(w_output.shape, BF16),
        pltpu.VMEM((1, width), BF16),
        pltpu.VMEM(router_group.shape, BF16),
        pltpu.VMEM(router_expert.shape, BF16),
        pltpu.VMEM(expert_ids.shape, jnp.int32),
        pltpu.VMEM((width, 2 * ff), BF16),
        pltpu.VMEM((ff, width), BF16),
        dma((17,)),
        dma((1,)),
        pltpu.VMEM((n, seqs, a_cols), BF16),
        pltpu.VMEM((n, seqs, span), BF16),
        pltpu.VMEM((n, seqs, span), BF16),
        pltpu.VMEM((seqs, vw), BF16),
        pltpu.VMEM((n, seqs, vw), BF16),
        pltpu.VMEM((t, tokens, out_cols), BF16),
        pltpu.VMEM((tokens, out_cols), BF16),
        pltpu.VMEM((n, tokens, out_cols), BF16),
        pltpu.VMEM((n, seqs, width), BF16),
        pltpu.VMEM((n, seqs, width), BF16),
        pltpu.VMEM((t, seqs, width), BF16),
        pltpu.VMEM((seqs, width), BF16),
        pltpu.VMEM((seqs, width), F32),
        pltpu.VMEM((tokens, cols), F32),
        pltpu.VMEM((tokens, vw), F32),
        pltpu.VMEM((8, kw), F32),
        pltpu.VMEM((tokens, span), F32),
        pltpu.VMEM((tokens, width), F32),
        dma((5, n)),
        dma((5, n)),
        dma((2, t)),
        dma((2, t)),
    ]
    layer_out, new_state = pl.pallas_call(
        functools.partial(kernel, n, t),
        out_shape=(
            jax.ShapeDtypeStruct((seqs, width), BF16),
            jax.ShapeDtypeStruct(gla_state.shape, F32),
        ),
        in_specs=[pl.BlockSpec(memory_space=pl.ANY)] * len(operands),
        out_specs=(
            pl.BlockSpec(memory_space=pltpu.VMEM),
            pl.BlockSpec(memory_space=pl.ANY),
        ),
        scratch_shapes=scratch,
        compiler_params=pltpu.CompilerParams(
            collective_id=0, has_side_effects=True, vmem_limit_bytes=56 * 1024 * 1024
        ),
    )(*operands)
    return layer_out, new_state


def solution(mesh):
    n, t = mesh.shape["ep"], mesh.shape["tp"]
    placed = (
        P("ep", None),
        P("ep", "tp", None, None),
        P(),
        P("ep", "tp"),
        P("ep", "tp"),
        P("ep", "tp"),
        P("ep", "tp"),
        P("tp"),
        P(),
        P("tp", "ep"),
        P(),
        P(),
        P(),
        P(),
        P("ep", None, "tp"),
        P("ep", None, "tp"),
        P("ep", "tp", None),
    )
    return jax.shard_map(
        functools.partial(on_device, n, t),
        mesh=mesh,
        in_specs=placed,
        out_specs=(P("ep", None), P("ep", "tp", None, None)),
        check_vma=False,
    )
```

```python
import functools

import jax
import jax.numpy as jnp
from jax import lax
from jax.experimental import pallas as pl
from jax.experimental.pallas import tpu as pltpu
from jax.sharding import PartitionSpec as P

EPSILON = 1e-06
GATE_SCALE = 16.0
F32 = jnp.float32
BF16 = jnp.bfloat16
LANES = 128
MESH = pl.DeviceIdType.MESH


def mm(left, right):
    return jnp.dot(left, right, preferred_element_type=F32)


def mm_nt(left, right):
    return lax.dot_general(
        left, right, (((1,), (1,)), ((), ())), preferred_element_type=F32
    )


def over_peers(me, count, body, far_first=False):
    if count <= 8:
        order = range(1, count)
        for d in reversed(order) if far_first else order:
            body(flip(me, count, d))
    else:

        def step(d, carry):
            body(lax.rem(me + d, count))
            return carry

        lax.fori_loop(1, count, step, 0)


def flip(me, count, d):
    if count & (count - 1):
        return lax.rem(me + d, count)
    peer = me
    bit = 1
    while bit < count:
        if d & bit:
            peer = peer + bit - 2 * bit * ((me // bit) % 2)
        bit *= 2
    return peer


def over_range(count, body):
    for i in range(count):
        body(i)


def take_cols(ref, index, cols):
    if cols % LANES == 0:
        return ref[:, pl.ds(pl.multiple_of(index * cols, LANES), cols)]
    rows = ref.shape[1]
    select = (
        lax.broadcasted_iota(jnp.int32, (rows, cols), 0)
        == lax.broadcasted_iota(jnp.int32, (rows, cols), 1) + index * cols
    )
    return mm(ref[...].astype(BF16), jnp.where(select, 1.0, 0.0).astype(BF16)).astype(BF16)


def as_row(ref):
    values = ref[...].astype(F32)
    return jnp.concatenate([values[r : r + 1] for r in range(values.shape[0])], axis=1)


def kernel(
    n,
    t,
    residual_in,
    gla_state,
    norm_gain,
    w_query,
    w_key,
    w_value,
    w_decay,
    decay_bias,
    head_gain,
    w_output,
    ffn_gain,
    router_group,
    router_expert,
    expert_ids,
    w_gate,
    w_up,
    w_down,
    layer_out,
    new_state,
    res,
    state,
    ng,
    ng_row,
    wcat,
    bias,
    hg,
    wo,
    fg,
    fg_row,
    rg,
    re,
    ids,
    wgu,
    wd,
    load_sem,
    out_sem,
    a_rx,
    b_tx,
    b_rx,
    c_tx,
    c_rx,
    d1_rx,
    d1_tx,
    d2_rx,
    f1_tx,
    f1_rx,
    f2_rx,
    f2_tx,
    lout,
    rows_a,
    rows_c,
    heads8,
    proj,
    moe_out,
    ep_send,
    ep_recv,
    tp_send,
    tp_recv,
):
    e = lax.axis_index("ep")
    h = lax.axis_index("tp")
    seqs, width = res.shape
    cols = wcat.shape[0]
    kw = w_query.shape[1]
    vw = w_value.shape[1]
    tokens = n * seqs
    ff = wd.shape[0]
    aligned = cols % LANES == 0

    barrier = pltpu.get_barrier_semaphore()

    def greet(axis):
        return lambda peer: pl.semaphore_signal(
            barrier, inc=1, device_id={axis: peer}, device_id_type=MESH
        )

    over_peers(e, n, greet("ep"), far_first=True)
    over_peers(h, t, greet("tp"))

    loads = []

    def load(src, dst):
        copy = pltpu.make_async_copy(src, dst, load_sem.at[len(loads)])
        copy.start()
        loads.append(copy)
        return copy

    ld_res = load(residual_in, res)
    ld_ng = load(norm_gain, ng)
    ld_w = [
        load(w_query, wcat.at[:, 0:kw]),
        load(w_key, wcat.at[:, kw : 2 * kw]),
        load(w_value, wcat.at[:, 2 * kw : 2 * kw + vw]),
        load(w_decay, wcat.at[:, 2 * kw + vw :]),
    ]
    ld_small = [load(decay_bias, bias), load(head_gain, hg), load(ffn_gain, fg)]
    ld_state = load(gla_state.at[:, 0], state)
    ld_wo = load(w_output, wo)
    ld_route = [load(router_group, rg), load(router_expert, re), load(expert_ids, ids)]
    ld_gu = [load(w_gate.at[0], wgu.at[:, 0:ff]), load(w_up.at[0], wgu.at[:, ff : 2 * ff])]
    ld_wd = load(w_down.at[0], wd)

    def ep_copy(phase, src, dst, peer, slot):
        return pltpu.make_async_remote_copy(
            src_ref=src,
            dst_ref=dst,
            send_sem=ep_send.at[phase, peer],
            recv_sem=ep_recv.at[phase, slot],
            device_id={"ep": peer},
            device_id_type=MESH,
        )

    def tp_copy(phase, src, dst, peer, slot):
        return pltpu.make_async_remote_copy(
            src_ref=src,
            dst_ref=dst,
            send_sem=tp_send.at[phase, peer],
            recv_sem=tp_recv.at[phase, slot],
            device_id={"tp": peer},
            device_id_type=MESH,
        )

    def ep_src(tx):
        return lambda peer: tx.at[peer]

    def ep_phase_send(phase, src_of, rx):
        over_peers(
            e,
            n,
            lambda peer: ep_copy(phase, src_of(peer), rx.at[e], peer, e).start(),
            far_first=True,
        )

    def ep_wait(phase, rx, peer):
        ep_copy(phase, rx.at[peer], rx.at[peer], peer, peer).wait_recv()

    def ep_wait_all(phase, rx):
        over_peers(e, n, lambda peer: ep_wait(phase, rx, peer))

    def ep_drain(phase, src_of, rx):
        over_peers(
            e, n, lambda peer: ep_copy(phase, src_of(peer), rx.at[e], peer, e).wait_send()
        )

    def tp_phase_send(phase, src, rx):
        over_peers(
            h, t, lambda peer: tp_copy(phase, src, rx.at[h], peer, h).start(), far_first=True
        )

    def tp_wait_all(phase, rx):
        over_peers(
            h, t, lambda peer: tp_copy(phase, rx.at[peer], rx.at[peer], peer, peer).wait_recv()
        )

    def tp_drain(phase, src, rx):
        over_peers(
            h, t, lambda peer: tp_copy(phase, src, rx.at[h], peer, h).wait_send()
        )

    if aligned:
        a_src = lambda peer: res.at[:, pl.ds(pl.multiple_of(peer * cols, LANES), cols)]
    else:
        a_src = lambda peer: res
    ld_res.wait()
    pl.semaphore_wait(barrier, n - 1 + t - 1)
    ep_phase_send(0, a_src, a_rx)
    own = res[...]
    a_rx[e] = take_cols(res, e, cols) if aligned else own
    own_float = own.astype(F32)
    token_scale = lax.rsqrt(jnp.mean(own_float * own_float, axis=-1, keepdims=True) + EPSILON)
    ld_ng.wait()
    ng_row[...] = as_row(ng)
    ng_cols = take_cols(ng_row, e, cols).astype(F32)
    for copy in ld_w:
        copy.wait()
    ep_wait_all(0, a_rx)

    def fill_a(i):
        if aligned:
            piece = a_rx[i]
        else:
            piece = take_cols(a_rx.at[i], e, cols)
        rows_a[pl.ds(i * seqs, seqs), :] = piece.astype(F32)

    over_range(n, fill_a)

    lhs = (rows_a[...] * ng_cols).astype(BF16)
    proj[...] = mm(lhs, wcat[...])

    def fill_b(i):
        b_tx[i] = proj[pl.ds(i * seqs, seqs), :].astype(BF16)

    over_range(n, fill_b)
    ep_phase_send(1, ep_src(b_tx), b_rx)
    for copy in ld_small:
        copy.wait()
    ld_state.wait()
    for copy in ld_route + ld_gu:
        copy.wait()
    fg_row[...] = as_row(fg)
    b_rx[e] = b_tx[e]
    ep_wait_all(1, b_rx)
    total = jnp.sum(b_rx[...].astype(F32), axis=0) * token_scale

    heads8[...] = jnp.zeros_like(heads8)
    decay_pre = total[:, 2 * kw + vw :] + bias[...]
    log_decay = (
        jnp.minimum(decay_pre, 0.0) - jnp.log1p(jnp.exp(-jnp.abs(decay_pre)))
    ) / GATE_SCALE
    heads8[0:seqs, :] = total[:, 0:kw] * kw ** (-0.5)
    heads8[seqs : 2 * seqs, :] = total[:, kw : 2 * kw]
    heads8[2 * seqs : 3 * seqs, :] = jnp.exp(log_decay)
    turned = heads8[...].T
    head_row = as_row(hg)
    value_rows = total[:, 2 * kw : 2 * kw + vw]
    for b in range(seqs):
        value = value_rows[b : b + 1]
        acc = jnp.zeros((8, vw), F32)
        chunk = 64
        for c in range(0, kw, chunk):
            q_col = turned[c : c + chunk, b : b + 1]
            k_col = turned[c : c + chunk, seqs + b : seqs + b + 1]
            a_col = turned[c : c + chunk, 2 * seqs + b : 2 * seqs + b + 1]
            fresh = a_col * state[b, c : c + chunk, :] + k_col * value
            state[b, c : c + chunk, :] = fresh
            acc = acc + jnp.sum((q_col * fresh).reshape(chunk // 8, 8, vw), axis=0)
        read = jnp.sum(acc, axis=0, keepdims=True)
        gated = read * lax.rsqrt(jnp.mean(read * read, axis=-1, keepdims=True) + EPSILON)
        gated = gated * head_row
        rows_c[b : b + 1, :] = gated
    c_tx[...] = rows_c[0:seqs, :].astype(BF16)

    c_src = lambda peer: c_tx
    ep_phase_send(2, c_src, c_rx)
    st_out = pltpu.make_async_copy(state, new_state.at[:, 0], out_sem.at[0])
    st_out.start()
    c_rx[e] = c_tx[...]
    ld_wo.wait()
    ep_wait_all(2, c_rx)

    def fill_c(i):
        rows_c[pl.ds(i * seqs, seqs), :] = c_rx[i].astype(F32)

    over_range(n, fill_c)

    part = mm(rows_c[...].astype(BF16), wo[...]).astype(BF16)
    d1_tx[...] = part
    tp_phase_send(0, d1_tx, d1_rx)
    d1_rx[h] = part
    tp_wait_all(0, d1_rx)
    attention = jnp.sum(d1_rx[...].astype(F32), axis=0)
    hid = (rows_a[...] + attention).astype(BF16)
    d2_rx[e] = hid
    d2_src = lambda peer: d2_rx.at[e]
    ep_phase_send(3, d2_src, d2_rx)

    square = jnp.zeros((tokens, 1), F32)
    gate_up = jnp.zeros((tokens, 2 * ff), F32)
    group_logits = jnp.zeros((tokens, rg.shape[0]), F32)
    expert_logits = jnp.zeros((tokens, re.shape[0]), F32)

    def moe_chunk(src, carry):
        square, gate_up, group_logits, expert_logits = carry
        piece = d2_rx[src].astype(F32)
        square = square + jnp.sum(piece * piece, axis=-1, keepdims=True)
        piece = (piece * take_cols(fg_row, src, cols).astype(F32)).astype(BF16)
        span = pl.ds(pl.multiple_of(src * cols, cols), cols)
        gate_up = gate_up + mm(piece, wgu[span, :])
        group_logits = group_logits + mm_nt(piece, take_cols(rg, src, cols))
        expert_logits = expert_logits + mm_nt(piece, take_cols(re, src, cols))
        return square, gate_up, group_logits, expert_logits

    def moe_step(src, carry):
        ep_wait(3, d2_rx, src)
        return moe_chunk(src, carry)

    carry = moe_chunk(e, (square, gate_up, group_logits, expert_logits))
    if n <= 8:
        for d in range(1, n):
            carry = moe_step(flip(e, n, d), carry)
    else:
        carry = lax.fori_loop(1, n, lambda d, c: moe_step(lax.rem(e + d, n), c), carry)
    square, gate_up, group_logits, expert_logits = carry
    scale = lax.rsqrt(square / (n * cols) + EPSILON)
    gate_up = gate_up * scale
    group_logits = group_logits * scale
    expert_logits = expert_logits * scale

    groups = group_logits.shape[1]
    experts = expert_logits.shape[1]
    diagonal = lax.broadcasted_iota(jnp.int32, (tokens, tokens), 0) == (
        lax.broadcasted_iota(jnp.int32, (tokens, tokens), 1)
    )
    column = lambda row: jnp.sum(jnp.where(diagonal, row, 0), axis=1, keepdims=True)
    first, second = column(ids[0:1, :]), column(ids[1:2, :])
    named = (first == e) | (second == e)
    rival = jnp.where(first == e, second, first)
    expert_at = lax.broadcasted_iota(jnp.int32, expert_logits.shape, 1)
    group_at = lax.broadcasted_iota(jnp.int32, group_logits.shape, 1)
    pick = lambda mask, values: jnp.sum(jnp.where(mask, values, 0.0), axis=1, keepdims=True)
    chosen = pick(expert_at == e, expert_logits)
    rival_logit = pick(expert_at == rival, expert_logits)
    group_logit = pick(group_at == e // (experts // groups), group_logits)
    share = 1.0 / jnp.sum(jnp.exp(group_logits - group_logit), axis=1, keepdims=True)
    weight = jnp.where(named, share / (1.0 + jnp.exp(rival_logit - chosen)), 0.0)

    gate, up = gate_up[:, 0:ff], gate_up[:, ff : 2 * ff]
    hidden = (gate / (1.0 + jnp.exp(-gate)) * up).astype(BF16)
    ld_wd.wait()
    moe_out[...] = mm(hidden, wd[...]) * weight

    def fill_f(i):
        f1_tx[i] = moe_out[pl.ds(i * seqs, seqs), :].astype(BF16)

    over_range(n, fill_f)
    f1_src = ep_src(f1_tx)
    ep_phase_send(4, f1_src, f1_rx)
    f1_rx[e] = f1_tx[e]
    ep_drain(0, a_src, a_rx)
    own_rows = (
        lax.broadcasted_iota(jnp.int32, (8, tokens), 1)
        == lax.broadcasted_iota(jnp.int32, (8, tokens), 0) + e * seqs
    )
    own_rows = jnp.where(own_rows, 1.0, 0.0).astype(BF16)
    if aligned:
        for i in range(n):
            lout[:, i * cols : (i + 1) * cols] = mm(own_rows, d2_rx[i])[0:seqs]
    ep_wait_all(4, f1_rx)
    f2_tx[...] = jnp.sum(f1_rx[...].astype(F32), axis=0).astype(BF16)
    tp_phase_send(1, f2_tx, f2_rx)
    f2_rx[h] = f2_tx[...]
    tp_wait_all(1, f2_rx)
    if not aligned:

        def place(i, total_rows):
            rows = mm(own_rows, d2_rx[i]).astype(BF16)
            select = (
                lax.broadcasted_iota(jnp.int32, (cols, width), 1)
                == lax.broadcasted_iota(jnp.int32, (cols, width), 0) + i * cols
            )
            return total_rows + mm(rows, jnp.where(select, 1.0, 0.0).astype(BF16))

        lout[...] = lax.fori_loop(0, n, place, jnp.zeros((8, width), F32))[0:seqs]
    moe_sum = jnp.sum(f2_rx[...].astype(F32), axis=0)
    res[...] = (lout[...] + moe_sum).astype(BF16)
    lo_out = pltpu.make_async_copy(res, layer_out, out_sem.at[1])
    lo_out.start()

    ep_drain(1, ep_src(b_tx), b_rx)
    ep_drain(2, c_src, c_rx)
    ep_drain(3, d2_src, d2_rx)
    ep_drain(4, f1_src, f1_rx)
    tp_drain(0, d1_tx, d1_rx)
    tp_drain(1, f2_tx, f2_rx)
    st_out.wait()
    lo_out.wait()


def on_device(n, t, *arrays):
    (
        residual_in,
        gla_state,
        norm_gain,
        w_query,
        w_key,
        w_value,
        w_decay,
        decay_bias,
        head_gain,
        w_output,
        ffn_gain,
        router_group,
        router_expert,
        expert_ids,
        w_gate,
        w_up,
        w_down,
    ) = arrays
    seqs, width = residual_in.shape
    tokens = n * seqs
    cols, kw = w_query.shape
    vw = w_value.shape[1]
    ff = w_gate.shape[2]
    span = 3 * kw + vw
    out_cols = w_output.shape[1]
    a_cols = cols if cols % LANES == 0 else width
    lanes = lambda a: a.reshape(-1, LANES)
    operands = (
        residual_in,
        gla_state,
        lanes(norm_gain),
        w_query,
        w_key,
        w_value,
        w_decay,
        decay_bias.reshape(1, -1),
        lanes(head_gain),
        w_output,
        lanes(ffn_gain),
        router_group.T,
        router_expert,
        expert_ids.T,
        w_gate,
        w_up,
        w_down,
    )
    dma = pltpu.SemaphoreType.DMA
    scratch = [
        pltpu.VMEM((seqs, width), BF16),
        pltpu.VMEM((seqs, kw, vw), F32),
        pltpu.VMEM((width // LANES, LANES), BF16),
        pltpu.VMEM((1, width), F32),
        pltpu.VMEM((cols, span), BF16),
        pltpu.VMEM((1, kw), F32),
        pltpu.VMEM((vw // LANES, LANES), BF16),
        pltpu.VMEM(w_output.shape, BF16),
        pltpu.VMEM((width // LANES, LANES), BF16),
        pltpu.VMEM((1, width), F32),
        pltpu.VMEM(router_group.shape[::-1], BF16),
        pltpu.VMEM(router_expert.shape, BF16),
        pltpu.VMEM(expert_ids.shape[::-1], jnp.int32),
        pltpu.VMEM((width, 2 * ff), BF16),
        pltpu.VMEM((ff, width), BF16),
        dma((17,)),
        dma((2,)),
        pltpu.VMEM((n, seqs, a_cols), BF16),
        pltpu.VMEM((n, seqs, span), BF16),
        pltpu.VMEM((n, seqs, span), BF16),
        pltpu.VMEM((seqs, vw), BF16),
        pltpu.VMEM((n, seqs, vw), BF16),
        pltpu.VMEM((t, tokens, out_cols), BF16),
        pltpu.VMEM((tokens, out_cols), BF16),
        pltpu.VMEM((n, tokens, out_cols), BF16),
        pltpu.VMEM((n, seqs, width), BF16),
        pltpu.VMEM((n, seqs, width), BF16),
        pltpu.VMEM((t, seqs, width), BF16),
        pltpu.VMEM((seqs, width), BF16),
        pltpu.VMEM((seqs, width), F32),
        pltpu.VMEM((tokens, cols), F32),
        pltpu.VMEM((tokens, vw), F32),
        pltpu.VMEM((8, kw), F32),
        pltpu.VMEM((tokens, span), F32),
        pltpu.VMEM((tokens, width), F32),
        dma((5, n)),
        dma((5, n)),
        dma((2, t)),
        dma((2, t)),
    ]
    limit = (12 if n <= 8 else 48) * 1024 * 1024
    layer_out, new_state = pl.pallas_call(
        functools.partial(kernel, n, t),
        out_shape=(
            jax.ShapeDtypeStruct((seqs, width), BF16),
            jax.ShapeDtypeStruct(gla_state.shape, F32),
        ),
        in_specs=[pl.BlockSpec(memory_space=pltpu.HBM)] * len(operands),
        out_specs=(
            pl.BlockSpec(memory_space=pl.ANY),
            pl.BlockSpec(memory_space=pl.ANY),
        ),
        scratch_shapes=scratch,
        compiler_params=pltpu.CompilerParams(
            collective_id=0, has_side_effects=True, vmem_limit_bytes=limit
        ),
    )(*[pltpu.with_memory_space_constraint(a, pltpu.HBM) for a in operands])
    return layer_out, new_state


def solution(mesh):
    n, t = mesh.shape["ep"], mesh.shape["tp"]
    placed = (
        P("ep", None),
        P("ep", "tp", None, None),
        P(),
        P("ep", "tp"),
        P("ep", "tp"),
        P("ep", "tp"),
        P("ep", "tp"),
        P("tp"),
        P(),
        P("tp", "ep"),
        P(),
        P(),
        P(),
        P(),
        P("ep", None, "tp"),
        P("ep", None, "tp"),
        P("ep", "tp", None),
    )
    return jax.shard_map(
        functools.partial(on_device, n, t),
        mesh=mesh,
        in_specs=placed,
        out_specs=(P("ep", None), P("ep", "tp", None, None)),
        check_vma=False,
    )
```

```python
import functools

import jax
import jax.numpy as jnp
from jax import lax
from jax.experimental import pallas as pl
from jax.experimental.pallas import tpu as pltpu
from jax.sharding import PartitionSpec as P

EPSILON = 1e-06
GATE_SCALE = 16.0
F32 = jnp.float32
BF16 = jnp.bfloat16
LANES = 128
MESH = pl.DeviceIdType.MESH


def mm(left, right):
    return jnp.dot(left, right, preferred_element_type=F32)


def over_peers(me, count, body, far_first=False):
    if count <= 8:
        order = range(1, count)
        for d in reversed(order) if far_first else order:
            body(flip(me, count, d))
    else:

        def step(d, carry):
            body(lax.rem(me + d, count))
            return carry

        lax.fori_loop(1, count, step, 0)


def flip(me, count, d):
    if count & (count - 1):
        return lax.rem(me + d, count)
    peer = me
    bit = 1
    while bit < count:
        if d & bit:
            peer = peer + bit - 2 * bit * ((me // bit) % 2)
        bit *= 2
    return peer


def over_range(count, body):
    for i in range(count):
        body(i)


def take_cols(ref, index, cols):
    if cols % LANES == 0:
        return ref[:, pl.ds(pl.multiple_of(index * cols, LANES), cols)]
    rows = ref.shape[1]
    select = (
        lax.broadcasted_iota(jnp.int32, (rows, cols), 0)
        == lax.broadcasted_iota(jnp.int32, (rows, cols), 1) + index * cols
    )
    return mm(ref[...].astype(BF16), jnp.where(select, 1.0, 0.0).astype(BF16)).astype(BF16)


def as_row(ref):
    values = ref[...].astype(F32)
    return jnp.concatenate([values[r : r + 1] for r in range(values.shape[0])], axis=1)


def kernel(
    n,
    t,
    residual_in,
    gla_state,
    norm_gain,
    w_query,
    w_key,
    w_value,
    w_decay,
    decay_bias,
    head_gain,
    w_output,
    ffn_gain,
    router_group,
    router_expert,
    expert_ids,
    w_gate,
    w_up,
    w_down,
    layer_out,
    new_state,
    res,
    state,
    ng,
    ng_row,
    wcat,
    bias,
    hg,
    wo,
    fg,
    fg_row,
    rg,
    re,
    both,
    route,
    ids,
    wgu,
    wd,
    load_sem,
    out_sem,
    a_rx,
    b_tx,
    b_rx,
    c_tx,
    c_rx,
    d1_rx,
    d1_tx,
    d2_tx,
    d2_rx,
    f1_tx,
    f1_rx,
    f2_rx,
    f2_tx,
    lout,
    rows_a,
    rows_c,
    heads8,
    proj,
    moe_out,
    ep_send,
    ep_recv,
    tp_send,
    tp_recv,
):
    e = lax.axis_index("ep")
    h = lax.axis_index("tp")
    seqs, width = res.shape
    cols = wcat.shape[0]
    kw = w_query.shape[1]
    vw = w_value.shape[1]
    tokens = n * seqs
    ff = wd.shape[0]
    aligned = cols % LANES == 0

    loads = []

    def load(src, dst):
        copy = pltpu.make_async_copy(src, dst, load_sem.at[len(loads)])
        copy.start()
        loads.append(copy)
        return copy

    ld_res = load(residual_in, res)

    barrier = pltpu.get_barrier_semaphore()

    def greet(axis):
        return lambda peer: pl.semaphore_signal(
            barrier, inc=1, device_id={axis: peer}, device_id_type=MESH
        )

    over_peers(e, n, greet("ep"), far_first=True)
    over_peers(h, t, greet("tp"))

    ld_ng = load(norm_gain, ng)
    ld_w = [
        load(w_query, wcat.at[:, 0:kw]),
        load(w_key, wcat.at[:, kw : 2 * kw]),
        load(w_value, wcat.at[:, 2 * kw : 2 * kw + vw]),
        load(w_decay, wcat.at[:, 2 * kw + vw :]),
    ]

    def ep_copy(phase, src, dst, peer, slot):
        return pltpu.make_async_remote_copy(
            src_ref=src,
            dst_ref=dst,
            send_sem=ep_send.at[phase, peer],
            recv_sem=ep_recv.at[phase, slot],
            device_id={"ep": peer},
            device_id_type=MESH,
        )

    def tp_copy(phase, src, dst, peer, slot):
        return pltpu.make_async_remote_copy(
            src_ref=src,
            dst_ref=dst,
            send_sem=tp_send.at[phase, peer],
            recv_sem=tp_recv.at[phase, slot],
            device_id={"tp": peer},
            device_id_type=MESH,
        )

    def ep_src(tx):
        return lambda peer: tx.at[peer]

    def ep_phase_send(phase, src_of, rx):
        over_peers(
            e,
            n,
            lambda peer: ep_copy(phase, src_of(peer), rx.at[e], peer, e).start(),
            far_first=True,
        )

    def ep_wait(phase, rx, peer):
        ep_copy(phase, rx.at[peer], rx.at[peer], peer, peer).wait_recv()

    def ep_wait_all(phase, rx):
        over_peers(e, n, lambda peer: ep_wait(phase, rx, peer))

    def ep_drain(phase, src_of, rx):
        over_peers(
            e, n, lambda peer: ep_copy(phase, src_of(peer), rx.at[e], peer, e).wait_send()
        )

    def tp_phase_send(phase, src, rx):
        over_peers(
            h, t, lambda peer: tp_copy(phase, src, rx.at[h], peer, h).start(), far_first=True
        )

    def tp_wait_all(phase, rx):
        over_peers(
            h, t, lambda peer: tp_copy(phase, rx.at[peer], rx.at[peer], peer, peer).wait_recv()
        )

    def tp_drain(phase, src, rx):
        over_peers(
            h, t, lambda peer: tp_copy(phase, src, rx.at[h], peer, h).wait_send()
        )

    if aligned:
        a_src = lambda peer: res.at[:, pl.ds(pl.multiple_of(peer * cols, LANES), cols)]
    else:
        a_src = lambda peer: res
    ld_res.wait()
    pl.semaphore_wait(barrier, n - 1 + t - 1)
    ep_phase_send(0, a_src, a_rx)

    ld_small = [load(decay_bias, bias), load(head_gain, hg), load(ffn_gain, fg)]
    ld_state = load(gla_state.at[:, 0], state)
    ld_wo = load(w_output, wo)
    ld_route = [load(router_group, rg), load(router_expert, re), load(expert_ids, ids)]
    ld_gu = [load(w_gate.at[0], wgu.at[:, 0:ff]), load(w_up.at[0], wgu.at[:, ff : 2 * ff])]
    ld_wd = load(w_down.at[0], wd)
    own = res[...]
    a_rx[e] = take_cols(res, e, cols) if aligned else own
    own_float = own.astype(F32)
    token_scale = lax.rsqrt(jnp.mean(own_float * own_float, axis=-1, keepdims=True) + EPSILON)
    ld_ng.wait()
    ng_row[...] = as_row(ng)
    ng_cols = take_cols(ng_row, e, cols).astype(F32)
    for copy in ld_w:
        copy.wait()
    ep_wait_all(0, a_rx)

    def fill_a(i):
        if aligned:
            piece = a_rx[i]
        else:
            piece = take_cols(a_rx.at[i], e, cols)
        rows_a[pl.ds(i * seqs, seqs), :] = piece.astype(F32)

    over_range(n, fill_a)

    lhs = (rows_a[...] * ng_cols).astype(BF16)
    proj[...] = mm(lhs, wcat[...])

    def fill_b(i):
        b_tx[i] = proj[pl.ds(i * seqs, seqs), :].astype(BF16)

    over_range(n, fill_b)
    ep_phase_send(1, ep_src(b_tx), b_rx)
    for copy in ld_small:
        copy.wait()
    ld_state.wait()
    for copy in ld_route + ld_gu:
        copy.wait()
    fg_row[...] = as_row(fg)
    experts, groups = re.shape[0], rg.shape[0]
    both[...] = jnp.zeros_like(both)
    both[0:experts, :] = re[...].astype(F32)
    both[experts : experts + groups, :] = rg[...].astype(F32)
    route[...] = both[...].T.astype(BF16)
    b_rx[e] = b_tx[e]
    ep_wait_all(1, b_rx)
    total = jnp.sum(b_rx[...].astype(F32), axis=0) * token_scale

    heads8[...] = jnp.zeros_like(heads8)
    decay_pre = total[:, 2 * kw + vw :] + bias[...]
    log_decay = (
        jnp.minimum(decay_pre, 0.0) - jnp.log1p(jnp.exp(-jnp.abs(decay_pre)))
    ) / GATE_SCALE
    heads8[0:seqs, :] = total[:, 0:kw] * kw ** (-0.5)
    heads8[seqs : 2 * seqs, :] = total[:, kw : 2 * kw]
    heads8[2 * seqs : 3 * seqs, :] = jnp.exp(log_decay)
    turned = heads8[...].T
    head_row = as_row(hg)
    value_rows = total[:, 2 * kw : 2 * kw + vw]
    for b in range(seqs):
        value = value_rows[b : b + 1]
        acc = jnp.zeros((8, vw), F32)
        chunk = 64
        for c in range(0, kw, chunk):
            q_col = turned[c : c + chunk, b : b + 1]
            k_col = turned[c : c + chunk, seqs + b : seqs + b + 1]
            a_col = turned[c : c + chunk, 2 * seqs + b : 2 * seqs + b + 1]
            fresh = a_col * state[b, c : c + chunk, :] + k_col * value
            state[b, c : c + chunk, :] = fresh
            acc = acc + jnp.sum((q_col * fresh).reshape(chunk // 8, 8, vw), axis=0)
        read = jnp.sum(acc, axis=0, keepdims=True)
        gated = read * lax.rsqrt(jnp.mean(read * read, axis=-1, keepdims=True) + EPSILON)
        gated = gated * head_row
        rows_c[b : b + 1, :] = gated
    c_tx[...] = rows_c[0:seqs, :].astype(BF16)

    c_src = lambda peer: c_tx
    ep_phase_send(2, c_src, c_rx)
    st_out = pltpu.make_async_copy(state, new_state.at[:, 0], out_sem.at[0])
    st_out.start()
    c_rx[e] = c_tx[...]
    ld_wo.wait()
    ep_wait_all(2, c_rx)

    def fill_c(i):
        rows_c[pl.ds(i * seqs, seqs), :] = c_rx[i].astype(F32)

    over_range(n, fill_c)

    part = mm(rows_c[...].astype(BF16), wo[...]).astype(BF16)
    d1_tx[...] = part
    tp_phase_send(0, d1_tx, d1_rx)
    d1_rx[h] = part
    tp_wait_all(0, d1_rx)
    attention = jnp.sum(d1_rx[...].astype(F32), axis=0)
    hid = (rows_a[...] + attention).astype(BF16)
    d2_tx[...] = hid
    d2_src = lambda peer: d2_tx
    ep_phase_send(3, d2_src, d2_rx)
    d2_rx[e] = hid

    square = jnp.zeros((tokens, cols), F32)
    gate_up = jnp.zeros((tokens, 2 * ff), F32)
    logits = jnp.zeros((tokens, route.shape[1]), F32)

    def moe_chunk(src, carry):
        square, gate_up, logits = carry
        piece = d2_rx[src].astype(F32)
        square = square + piece * piece
        piece = (piece * take_cols(fg_row, src, cols).astype(F32)).astype(BF16)
        span = pl.ds(pl.multiple_of(src * cols, cols), cols)
        gate_up = gate_up + mm(piece, wgu[span, :])
        logits = logits + mm(piece, route[span, :])
        return square, gate_up, logits

    def moe_step(src, carry):
        ep_wait(3, d2_rx, src)
        return moe_chunk(src, carry)

    carry = moe_chunk(e, (square, gate_up, logits))
    if n <= 8:
        for part in (range(1, n // 2), range(n // 2, n)):
            for d in part:
                ep_wait(3, d2_rx, flip(e, n, d))
            for d in part:
                carry = moe_chunk(flip(e, n, d), carry)
    else:
        carry = lax.fori_loop(1, n, lambda d, c: moe_step(lax.rem(e + d, n), c), carry)
    square, gate_up, logits = carry
    square = jnp.sum(square, axis=-1, keepdims=True)
    scale = lax.rsqrt(square / (n * cols) + EPSILON)
    gate_up = gate_up * scale
    logits = logits * scale

    diagonal = lax.broadcasted_iota(jnp.int32, (tokens, tokens), 0) == (
        lax.broadcasted_iota(jnp.int32, (tokens, tokens), 1)
    )
    column = lambda row: jnp.sum(jnp.where(diagonal, row, 0), axis=1, keepdims=True)
    first, second = column(ids[0:1, :]), column(ids[1:2, :])
    named = (first == e) | (second == e)
    rival = jnp.where(first == e, second, first)
    at = lax.broadcasted_iota(jnp.int32, logits.shape, 1)
    pick = lambda mask, values: jnp.sum(jnp.where(mask, values, 0.0), axis=1, keepdims=True)
    chosen = pick(at == e, logits)
    rival_logit = pick(at == rival, logits)
    group_logit = pick(at == experts + e // (experts // groups), logits)
    is_group = (at >= experts) & (at < experts + groups)
    shifted = jnp.where(is_group, logits - group_logit, 0.0)
    share = 1.0 / pick(is_group, jnp.exp(shifted))
    weight = jnp.where(named, share / (1.0 + jnp.exp(rival_logit - chosen)), 0.0)

    gate, up = gate_up[:, 0:ff], gate_up[:, ff : 2 * ff]
    hidden = (gate / (1.0 + jnp.exp(-gate)) * up).astype(BF16)
    ld_wd.wait()
    moe_out[...] = mm(hidden, wd[...]) * weight

    def fill_f(i):
        f1_tx[i] = moe_out[pl.ds(i * seqs, seqs), :].astype(BF16)

    over_range(n, fill_f)
    f1_src = ep_src(f1_tx)
    ep_phase_send(4, f1_src, f1_rx)
    f1_rx[e] = f1_tx[e]
    ep_drain(0, a_src, a_rx)
    own_rows = (
        lax.broadcasted_iota(jnp.int32, (8, tokens), 1)
        == lax.broadcasted_iota(jnp.int32, (8, tokens), 0) + e * seqs
    )
    own_rows = jnp.where(own_rows, 1.0, 0.0).astype(BF16)
    if aligned:
        for i in range(n):
            lout[:, i * cols : (i + 1) * cols] = mm(own_rows, d2_rx[i])[0:seqs]
    ep_wait_all(4, f1_rx)
    f2_tx[...] = jnp.sum(f1_rx[...].astype(F32), axis=0).astype(BF16)
    tp_phase_send(1, f2_tx, f2_rx)
    f2_rx[h] = f2_tx[...]
    tp_wait_all(1, f2_rx)
    if not aligned:

        def place(i, total_rows):
            rows = mm(own_rows, d2_rx[i]).astype(BF16)
            select = (
                lax.broadcasted_iota(jnp.int32, (cols, width), 1)
                == lax.broadcasted_iota(jnp.int32, (cols, width), 0) + i * cols
            )
            return total_rows + mm(rows, jnp.where(select, 1.0, 0.0).astype(BF16))

        lout[...] = lax.fori_loop(0, n, place, jnp.zeros((8, width), F32))[0:seqs]
    moe_sum = jnp.sum(f2_rx[...].astype(F32), axis=0)
    res[...] = (lout[...] + moe_sum).astype(BF16)
    lo_out = pltpu.make_async_copy(res, layer_out, out_sem.at[1])
    lo_out.start()

    ep_drain(1, ep_src(b_tx), b_rx)
    ep_drain(2, c_src, c_rx)
    ep_drain(3, d2_src, d2_rx)
    ep_drain(4, f1_src, f1_rx)
    tp_drain(0, d1_tx, d1_rx)
    tp_drain(1, f2_tx, f2_rx)
    st_out.wait()
    lo_out.wait()


def on_device(n, t, *arrays):
    (
        residual_in,
        gla_state,
        norm_gain,
        w_query,
        w_key,
        w_value,
        w_decay,
        decay_bias,
        head_gain,
        w_output,
        ffn_gain,
        router_group,
        router_expert,
        expert_ids,
        w_gate,
        w_up,
        w_down,
    ) = arrays
    seqs, width = residual_in.shape
    tokens = n * seqs
    cols, kw = w_query.shape
    vw = w_value.shape[1]
    ff = w_gate.shape[2]
    span = 3 * kw + vw
    out_cols = w_output.shape[1]
    a_cols = cols if cols % LANES == 0 else width
    lanes = lambda a: a.reshape(-1, LANES)
    operands = (
        residual_in,
        gla_state,
        lanes(norm_gain),
        w_query,
        w_key,
        w_value,
        w_decay,
        decay_bias.reshape(1, -1),
        lanes(head_gain),
        w_output,
        lanes(ffn_gain),
        router_group.T,
        router_expert,
        expert_ids.T,
        w_gate,
        w_up,
        w_down,
    )
    route_cols = -(-(router_expert.shape[0] + router_group.shape[1]) // LANES) * LANES
    dma = pltpu.SemaphoreType.DMA
    scratch = [
        pltpu.VMEM((seqs, width), BF16),
        pltpu.VMEM((seqs, kw, vw), F32),
        pltpu.VMEM((width // LANES, LANES), BF16),
        pltpu.VMEM((1, width), F32),
        pltpu.VMEM((cols, span), BF16),
        pltpu.VMEM((1, kw), F32),
        pltpu.VMEM((vw // LANES, LANES), BF16),
        pltpu.VMEM(w_output.shape, BF16),
        pltpu.VMEM((width // LANES, LANES), BF16),
        pltpu.VMEM((1, width), F32),
        pltpu.VMEM(router_group.shape[::-1], BF16),
        pltpu.VMEM(router_expert.shape, BF16),
        pltpu.VMEM((route_cols, width), F32),
        pltpu.VMEM((width, route_cols), BF16),
        pltpu.VMEM(expert_ids.shape[::-1], jnp.int32),
        pltpu.VMEM((width, 2 * ff), BF16),
        pltpu.VMEM((ff, width), BF16),
        dma((17,)),
        dma((2,)),
        pltpu.VMEM((n, seqs, a_cols), BF16),
        pltpu.VMEM((n, seqs, span), BF16),
        pltpu.VMEM((n, seqs, span), BF16),
        pltpu.VMEM((seqs, vw), BF16),
        pltpu.VMEM((n, seqs, vw), BF16),
        pltpu.VMEM((t, tokens, out_cols), BF16),
        pltpu.VMEM((tokens, out_cols), BF16),
        pltpu.VMEM((tokens, out_cols), BF16),
        pltpu.VMEM((n, tokens, out_cols), BF16),
        pltpu.VMEM((n, seqs, width), BF16),
        pltpu.VMEM((n, seqs, width), BF16),
        pltpu.VMEM((t, seqs, width), BF16),
        pltpu.VMEM((seqs, width), BF16),
        pltpu.VMEM((seqs, width), F32),
        pltpu.VMEM((tokens, cols), F32),
        pltpu.VMEM((tokens, vw), F32),
        pltpu.VMEM((8, kw), F32),
        pltpu.VMEM((tokens, span), F32),
        pltpu.VMEM((tokens, width), F32),
        dma((5, n)),
        dma((5, n)),
        dma((2, t)),
        dma((2, t)),
    ]
    limit = (12 if n <= 8 else 48) * 1024 * 1024
    layer_out, new_state = pl.pallas_call(
        functools.partial(kernel, n, t),
        out_shape=(
            jax.ShapeDtypeStruct((seqs, width), BF16),
            jax.ShapeDtypeStruct(gla_state.shape, F32),
        ),
        in_specs=[pl.BlockSpec(memory_space=pltpu.HBM)] * len(operands),
        out_specs=(
            pl.BlockSpec(memory_space=pl.ANY),
            pl.BlockSpec(memory_space=pl.ANY),
        ),
        scratch_shapes=scratch,
        compiler_params=pltpu.CompilerParams(
            collective_id=0, has_side_effects=True, vmem_limit_bytes=limit
        ),
    )(*[pltpu.with_memory_space_constraint(a, pltpu.HBM) for a in operands])
    return layer_out, new_state


def solution(mesh):
    n, t = mesh.shape["ep"], mesh.shape["tp"]
    placed = (
        P("ep", None),
        P("ep", "tp", None, None),
        P(),
        P("ep", "tp"),
        P("ep", "tp"),
        P("ep", "tp"),
        P("ep", "tp"),
        P("tp"),
        P(),
        P("tp", "ep"),
        P(),
        P(),
        P(),
        P(),
        P("ep", None, "tp"),
        P("ep", None, "tp"),
        P("ep", "tp", None),
    )
    return jax.shard_map(
        functools.partial(on_device, n, t),
        mesh=mesh,
        in_specs=placed,
        out_specs=(P("ep", None), P("ep", "tp", None, None)),
        check_vma=False,
    )
```
